32 devices in a mesh: sp: 16 (over z, y, x), dp: 2 (over core).
Axes of the slice: x: 2, y: 2, z: 4, core: 2. Of those that a mesh axis runs over, the one named last changes fastest.
Arguments:
- glu_value: bfloat16 [2, 8192, 512], P('dp', 'sp'), may hold values from -6 to 6
- glu_gate: bfloat16 [2, 8192, 512], P('dp', 'sp'), may hold values from -8 to 8
- cotangent: bfloat16 [2, 8192, 2048], P('dp', 'sp'), may hold values from -8 to 8
- conv_weight: float32 [31, 512], replicated, may hold values from -1 to 1
- norm_gain: float32 [512], replicated, may hold values from 0.1 to 1.9
- norm_shift: float32 [512], replicated, may hold values from -3 to 3
- out_weight: bfloat16 [2048, 512], P('dp'), may hold values from -0.25 to 0.25
Outputs:
- grad_value: bfloat16 [2, 8192, 512], P('dp', 'sp')
- grad_gate: bfloat16 [2, 8192, 512], P('dp', 'sp')
- grad_out_weight: float32 [2048, 512], P('dp')
- grad_conv: float32 [31, 512], replicated
- grad_gain: float32 [512], replicated
- grad_shift: float32 [512], replicated
The draws below stay inside these ranges and needn't reach their ends.
All inputs are finite; a program needn't handle non-finite values.
Results may differ from the reference program's by a relative error of at most 0.003.
Values may be sent and summed in bfloat16 or wider, within the bound.
A program may use at most 64 MiB of HBM per device.

```python
import math
import jax
import jax.numpy as jnp
from jax import lax

D = 2048
C = 512
SPAN = 31
SEQS = 2
LENGTH = 8192
TOKENS = 16384


def strengthened(drawn, stream_key, source, target, shards_of, factor):
    owner, partner = [(jnp.arange(drawn.shape[dim]) // (drawn.shape[dim] // shards_of)).reshape([-1 if axis == dim else 1 for axis in range(drawn.ndim)]) for dim in (source, target)]
    chosen = jax.random.permutation(stream_key, shards_of)[partner]
    strong = (owner == chosen) | (owner == (partner + shards_of // 2) % shards_of)
    return jnp.where(strong, factor * drawn, drawn)


def steps_of(stream_key, extent, split, low, high):
    def one(position, shards_of):
        heights = jax.random.uniform(jax.random.fold_in(jax.random.fold_in(stream_key, 6), position), (shards_of,), jnp.float32, low / len(split), high / len(split))
        return jnp.repeat(jnp.exp(heights), extent[position] // shards_of).reshape((-1,) + (1,) * (len(extent) - position - 1))

    gain = one(*split[0])
    for cut in split[1:]:
        gain = gain * one(*cut)
    return gain


def scatter_about(stream_key, dims, width, limit, cuts=(), held_as=jnp.bfloat16):
    drawn = width * jax.random.normal(stream_key, dims, jnp.float32)
    if cuts:
        drawn = drawn * steps_of(stream_key, dims, cuts, -0.22, 0.18)
    return jnp.clip(drawn, -limit, limit).astype(held_as)


def bell_draw_with(own_key, dims, width, bound, split, heavy, kind=jnp.bfloat16):
    values = width * jax.random.normal(own_key, dims, jnp.float32)
    if split:
        values = values * steps_of(own_key, dims, split, -0.22, 0.18)
    return jnp.clip(strengthened(values, jax.random.fold_in(own_key, 3), *heavy), -bound, bound).astype(kind)


def setup_inputs(seed: int = 0) -> dict:
    keys = jax.random.split(jax.random.key(seed), 8)
    return {
        "glu_value": scatter_about(keys[0], (SEQS, LENGTH, C), 1.0, 6.0, ((0, 2), (1, 16))),
        "glu_gate": scatter_about(keys[1], (SEQS, LENGTH, C), 1.5, 8.0, ((0, 2), (1, 16))),
        "cotangent": bell_draw_with(keys[2], (SEQS, LENGTH, D), 1.0, 8.0, ((0, 2), (1, 16)), (1, 2, 16, 2.0)),
        "conv_weight": scatter_about(keys[3], (SPAN, C), SPAN ** -0.5, 1.0, (), jnp.float32),
        "norm_gain": jnp.clip(1.0 + 0.18 * jax.random.normal(keys[4], (C,), jnp.float32), 0.1, 1.9),
        "norm_shift": scatter_about(keys[5], (C,), 0.5, 3.0, (), jnp.float32),
        "out_weight": scatter_about(keys[6], (D, C), C ** -0.5, 0.25, ((0, 2),)),
    }


epsilon = 1e-06

def sequence_grads(value_rows, gate_rows, cotan_rows, conv_weight, norm_gain, norm_shift, out_weight):
    length = value_rows.shape[0]
    channels = value_rows.shape[1]
    tap_count = conv_weight.shape[0]
    value_full = value_rows.astype(jnp.float32)
    gate_full = gate_rows.astype(jnp.float32)
    sigmoid_gate = jax.nn.sigmoid(gate_full)
    gated = value_full * sigmoid_gate
    padded = jnp.concatenate([jnp.zeros((tap_count - 1, channels), jnp.float32), gated], axis=0)
    conv_rows = jnp.zeros((length, channels), jnp.float32)
    for offset in range(tap_count):
        conv_rows = conv_rows + conv_weight[offset] * padded[offset:offset + length]
    centred = conv_rows - lax.optimization_barrier(jnp.mean(conv_rows, axis=-1, keepdims=True))
    inv_std = lax.rsqrt(lax.optimization_barrier(jnp.mean(centred * centred, axis=-1, keepdims=True)) + epsilon)
    normed = centred * inv_std
    pre_act = normed * norm_gain + norm_shift
    sigmoid_pre = jax.nn.sigmoid(pre_act)
    act_rows = (pre_act * sigmoid_pre).astype(jnp.bfloat16)
    grad_act = jnp.dot(cotan_rows, out_weight, preferred_element_type=jnp.float32)
    grad_pre = grad_act * sigmoid_pre * (1.0 + pre_act * (1.0 - sigmoid_pre))
    grad_normed = grad_pre * norm_gain
    grad_conv_rows = inv_std * (grad_normed - lax.optimization_barrier(jnp.mean(grad_normed, axis=-1, keepdims=True)) - normed * lax.optimization_barrier(jnp.mean(grad_normed * normed, axis=-1, keepdims=True)))
    padded_grad = jnp.concatenate([grad_conv_rows, jnp.zeros((tap_count - 1, channels), jnp.float32)], axis=0)
    grad_gated = jnp.zeros((length, channels), jnp.float32)
    for offset in range(tap_count):
        start = tap_count - 1 - offset
        grad_gated = grad_gated + conv_weight[offset] * padded_grad[start:start + length]
    grad_taps = jnp.stack([lax.optimization_barrier(jnp.sum(grad_conv_rows * padded[offset:offset + length], axis=0)) for offset in range(tap_count)], axis=0)
    grad_value = (grad_gated * sigmoid_gate).astype(jnp.bfloat16)
    grad_gate = (grad_gated * value_full * sigmoid_gate * (1.0 - sigmoid_gate)).astype(jnp.bfloat16)
    grad_weight = jnp.dot(cotan_rows.T, act_rows, preferred_element_type=jnp.float32)
    return (grad_value, grad_gate, grad_weight, grad_taps, lax.optimization_barrier(jnp.sum(grad_pre * normed, axis=0)), lax.optimization_barrier(jnp.sum(grad_pre, axis=0)))

def reference(glu_value, glu_gate, cotangent, conv_weight, norm_gain, norm_shift, out_weight):

    def one_sequence(items):
        return sequence_grads(items[0], items[1], items[2], conv_weight, norm_gain, norm_shift, out_weight)
    results = lax.map(one_sequence, (glu_value, glu_gate, cotangent))
    scale = 1.0 / math.sqrt(TOKENS)
    grad_out_weight = lax.optimization_barrier(jnp.sum(results[2], axis=0)) * scale
    grad_conv = lax.optimization_barrier(jnp.sum(results[3], axis=0)) * scale
    grad_gain = lax.optimization_barrier(jnp.sum(results[4], axis=0)) * scale
    grad_shift = lax.optimization_barrier(jnp.sum(results[5], axis=0)) * scale
    return (results[0], results[1], grad_out_weight, grad_conv, grad_gain, grad_shift)
```

```python
import functools
import math

import jax
import jax.numpy as jnp
from jax import lax
from jax.experimental import pallas as pl
from jax.experimental.pallas import tpu as pltpu
from jax.sharding import PartitionSpec as P

epsilon = 1e-06
LANES = 128
STREAMS = 4
NARROW_STAGES = 2
MAX_HALVINGS = 3
f32 = jnp.float32
bf16 = jnp.bfloat16


def flip(index, bit):
    size = 1 << bit
    here = (index // size) % 2
    return here, index + (1 - 2 * here) * size


def stage_plan(n_sp, rows):
    bits = int(math.log2(n_sp))
    plan = []
    for stage in range(bits):
        halve = stage < MAX_HALVINGS and rows // 2 >= 16
        plan.append((halve, rows))
        if halve:
            rows //= 2
    return plan, rows


def bit_order(n_sp, stream):
    order = list(range(int(math.log2(n_sp))))
    if stream % 2 and len(order) > 1:
        order[0], order[1] = order[1], order[0]
    return order


def kernel(
    n_sp, n_dp, plan,
    value, gate, cotan, taps, gain, shift, weight,
    grad_value, grad_gate, out_weight, out_small,
    gated, grads, normed, inv, act, grad_act, weights,
    halo_v, halo_g, edge_out, edge_in, sums, small, small_in,
    dp_out, dp_in, acc, narrow_out, narrow_in, wide_in, full_in, gathered,
    local_sem, w_send, w_recv, h_send, h_recv, dp_send, dp_recv, st_send, st_recv, sm_send, sm_recv,
):
    sp = lax.axis_index("sp")
    dp = lax.axis_index("dp")
    length, channels = value.shape
    tap_count = taps.shape[0]
    blocks = channels // LANES
    ext = grads.shape[1] - length
    lead = ext - (tap_count - 1)
    local_rows = weight.shape[0]
    streams, stream_rows = acc.shape[0], acc.shape[1]
    block_rows = min(64, length)
    row_blocks = length // block_rows
    sp_bits = int(math.log2(n_sp))
    dp_bits = int(math.log2(n_dp))
    later = (sp + 1) % n_sp
    prior = (sp + n_sp - 1) % n_sp

    barrier = pltpu.get_barrier_semaphore()
    partners = [{"sp": later}, {"sp": prior}]
    partners += [{"sp": flip(sp, b)[1]} for b in range(sp_bits)]
    partners += [{"dp": (dp + o) % n_dp} for o in range(1, n_dp)]
    for partner in partners:
        pl.semaphore_signal(barrier, inc=1, device_id=partner, device_id_type=pl.DeviceIdType.MESH)
    pl.semaphore_wait(barrier, len(partners))

    def remote(src, dst, send, recv, where):
        return pltpu.make_async_remote_copy(
            src_ref=src, dst_ref=dst, send_sem=send, recv_sem=recv,
            device_id=where, device_id_type=pl.DeviceIdType.MESH,
        )

    halos = [
        remote(value.at[pl.ds(length - ext, ext)], halo_v, h_send.at[0], h_recv.at[0], {"sp": later}),
        remote(gate.at[pl.ds(length - ext, ext)], halo_g, h_send.at[1], h_recv.at[1], {"sp": later}),
    ]
    for copy in halos:
        copy.start()
    own = pltpu.make_async_copy(weight, weights.at[dp], local_sem)
    own.start()
    w_copies = []
    for o in range(1, n_dp):
        w_copies.append(
            remote(weight, weights.at[dp], w_send.at[o - 1], w_recv.at[o - 1], {"dp": (dp + o) % n_dp})
        )
        w_copies[-1].start()

    def cols(b):
        return pl.ds(b * LANES, LANES)

    def gate_rows(v, g):
        return v.astype(f32) * jax.nn.sigmoid(g.astype(f32))

    def gating(i, _):
        r0 = pl.multiple_of(i * block_rows, block_rows)
        for b in range(blocks):
            gated[b, pl.ds(ext + r0, block_rows), :] = gate_rows(
                value[pl.ds(r0, block_rows), cols(b)], gate[pl.ds(r0, block_rows), cols(b)]
            )
        return 0

    lax.fori_loop(0, row_blocks, gating, 0)
    for copy in halos:
        copy.wait()
    for b in range(blocks):
        gated[b, 0:ext, :] = jnp.where(sp > 0, gate_rows(halo_v[:, cols(b)], halo_g[:, cols(b)]), 0.0)

    def row_mean(parts):
        total = parts[0]
        for p in parts[1:]:
            total = total + p
        return jnp.sum(total, axis=-1, keepdims=True) * (1.0 / channels)

    def forward(i, _):
        r0 = pl.multiple_of(i * block_rows, block_rows)
        rows = pl.ds(r0, block_rows)
        convs = []
        for b in range(blocks):
            total = jnp.zeros((block_rows, LANES), f32)
            for j in range(tap_count):
                total = total + taps[j : j + 1, cols(b)] * gated[b, pl.ds(r0 + lead + j, block_rows), :]
            convs.append(total)
        mean = row_mean(convs)
        centred = [c - mean for c in convs]
        inv_std = lax.rsqrt(row_mean([c * c for c in centred]) + epsilon)
        inv[rows, :] = inv_std
        for b in range(blocks):
            n = centred[b] * inv_std
            normed[rows, cols(b)] = n
            pre = n * gain[:, cols(b)] + shift[:, cols(b)]
            act[rows, cols(b)] = (pre * jax.nn.sigmoid(pre)).astype(bf16)
        return 0

    lax.fori_loop(0, row_blocks, forward, 0)

    dp_copies = [[None] * (n_dp - 1) for _ in range(streams)]

    def product(chunk, stream):
        start = pl.multiple_of(chunk * local_rows + stream * stream_rows, LANES)
        return lax.dot_general(
            cotan[:, pl.ds(start, stream_rows)], act[...], (((0,), (0,)), ((), ())),
            preferred_element_type=f32,
        )

    for k in range(streams):
        for o in range(1, n_dp):
            peer = (dp + o) % n_dp
            dp_out[o - 1, k] = product(peer, k)
            copy = remote(
                dp_out.at[o - 1, k], dp_in.at[o - 1, k],
                dp_send.at[k, o - 1], dp_recv.at[k, o - 1], {"dp": peer},
            )
            copy.start()
            dp_copies[k][o - 1] = copy
        acc[k] = product(dp, k)

    def exchange(k):
        order = bit_order(n_sp, k)
        for copy in dp_copies[k]:
            copy.wait()
        for o in range(1, n_dp):
            acc[k] += dp_in[o - 1, k]
        off = 0
        final = stream_rows
        for stage, (halve, rows) in enumerate(plan):
            here, partner = flip(sp, order[stage])
            sems = st_send.at[k, stage], st_recv.at[k, stage], {"sp": partner}
            if halve:
                half = rows // 2
                final = half
                spot = pl.ds(stream_rows - rows, half)
                out = pl.ds(pl.multiple_of(off + (1 - here) * half, half), half)
                off = off + here * half
                into = pl.ds(pl.multiple_of(off, half), half)
                if stage < NARROW_STAGES:
                    narrow_out[k, spot, :] = acc[k, out, :].astype(bf16)
                    copy = remote(narrow_out.at[k, spot], narrow_in.at[k, spot], *sems)
                    landed = narrow_in
                else:
                    copy = remote(acc.at[k, out], wide_in.at[k, spot], *sems)
                    landed = wide_in
                copy.start()
                yield
                copy.wait()
                acc[k, into, :] += landed[k, spot, :].astype(f32)
            else:
                into = pl.ds(pl.multiple_of(off, rows), rows)
                copy = remote(acc.at[k, into], full_in.at[k, stage], *sems)
                copy.start()
                yield
                copy.wait()
                acc[k, into, :] += full_in[k, stage]
        spot = pl.ds(pl.multiple_of(off, final), final)
        wide = pl.ds(pl.multiple_of(k * stream_rows + off, final), final)
        gathered[wide, :] = acc[k, spot, :].astype(bf16)
        for stage in reversed(range(len(plan))):
            halve, rows = plan[stage]
            if not halve:
                continue
            half = rows // 2
            here, partner = flip(sp, order[stage])
            spot = pl.ds(pl.multiple_of(k * stream_rows + off, half), half)
            back = len(plan) + stage
            copy = remote(
                gathered.at[spot], gathered.at[spot],
                st_send.at[k, back], st_recv.at[k, back], {"sp": partner},
            )
            copy.start()
            yield
            copy.wait()
            off = off - here * half
        out_weight[pl.ds(k * stream_rows, stream_rows), :] = gathered[pl.ds(k * stream_rows, stream_rows), :]

    def combine():
        step = 0
        axes = [("dp", dp, b) for b in range(dp_bits)] + [("sp", sp, b) for b in range(sp_bits)]
        for name, index, b in axes:
            copy = remote(small, small_in.at[step], sm_send.at[step], sm_recv.at[step], {name: flip(index, b)[1]})
            copy.start()
            yield
            copy.wait()
            small[...] += small_in[step]
            step += 1
        out_small[...] = small[...]

    flows = [exchange(k) for k in range(streams)]

    def advance():
        for flow in list(flows):
            if next(flow, "end") == "end":
                flows.remove(flow)

    for copy in w_copies:
        copy.wait()
    own.wait()
    total = None
    for d in range(n_dp):
        part = jnp.dot(cotan[:, d * local_rows : (d + 1) * local_rows], weights[d], preferred_element_type=f32)
        total = part if total is None else total + part
    grad_act[...] = total
    advance()
    sums[...] = jnp.zeros_like(sums)

    def backward(i):
        r0 = pl.multiple_of(i * block_rows, block_rows)
        rows = pl.ds(r0, block_rows)
        inv_std = inv[rows, :]
        normal, grad_normal = [], []
        for b in range(blocks):
            n = normed[rows, cols(b)]
            pre = n * gain[:, cols(b)] + shift[:, cols(b)]
            s = jax.nn.sigmoid(pre)
            grad_pre = grad_act[rows, cols(b)] * s * (1.0 + pre * (1.0 - s))
            sums[0, b] += jnp.sum((grad_pre * n).reshape(block_rows // 8, 8, LANES), axis=0)
            sums[1, b] += jnp.sum(grad_pre.reshape(block_rows // 8, 8, LANES), axis=0)
            normal.append(n)
            grad_normal.append(grad_pre * gain[:, cols(b)])
        first = row_mean(grad_normal)
        second = row_mean([g * n for g, n in zip(grad_normal, normal)])
        for b in range(blocks):
            grads[b, rows, :] = inv_std * (grad_normal[b] - first - normal[b] * second)

    backward(0)
    edge_out[...] = grads[:, 0:ext, :]
    edge = remote(edge_out, edge_in, h_send.at[2], h_recv.at[2], {"sp": prior})
    edge.start()

    def backward_loop(i, _):
        backward(i)
        return 0

    lax.fori_loop(1, row_blocks, backward_loop, 0)
    advance()

    small[...] = jnp.zeros_like(small)
    for b in range(blocks):

        def tap_rows(i, carry):
            r0 = pl.multiple_of(i * 8, 8)
            g = grads[b, pl.ds(r0, 8), :]
            return tuple(c + g * gated[b, pl.ds(r0 + lead + j, 8), :] for j, c in enumerate(carry))

        found = lax.fori_loop(
            0, length // 8, tap_rows, tuple(jnp.zeros((8, LANES), f32) for _ in range(tap_count))
        )
        for j in range(tap_count):
            small[j : j + 1, cols(b)] = jnp.sum(found[j], axis=0, keepdims=True)
        for row in range(2):
            small[tap_count + row : tap_count + row + 1, cols(b)] = jnp.sum(sums[row, b], axis=0, keepdims=True)
        if b % 2:
            advance()
    flows.insert(0, combine())
    edge.wait()
    for b in range(blocks):
        grads[b, pl.ds(length, ext), :] = jnp.where(sp < n_sp - 1, edge_in[b], 0.0)
    advance()

    def final_rows(i, _):
        r0 = pl.multiple_of(i * block_rows, block_rows)
        rows = pl.ds(r0, block_rows)
        for b in range(blocks):
            total = jnp.zeros((block_rows, LANES), f32)
            for j in range(tap_count):
                total = total + taps[j : j + 1, cols(b)] * grads[b, pl.ds(r0 + tap_count - 1 - j, block_rows), :]
            s = jax.nn.sigmoid(gate[rows, cols(b)].astype(f32))
            grad_value[rows, cols(b)] = (total * s).astype(bf16)
            grad_gate[rows, cols(b)] = (total * value[rows, cols(b)].astype(f32) * s * (1.0 - s)).astype(bf16)
        return 0

    pieces = math.gcd(row_blocks, 4)
    step = row_blocks // pieces
    for piece in range(pieces):
        lax.fori_loop(piece * step, (piece + 1) * step, final_rows, 0)
        advance()
    while flows:
        advance()


def per_device(glu_value, glu_gate, cotangent, conv_weight, norm_gain, norm_shift, out_weight):
    n_sp, n_dp = lax.axis_size("sp"), lax.axis_size("dp")
    length, channels = glu_value.shape[1:]
    features = cotangent.shape[2]
    tap_count = conv_weight.shape[0]
    local_rows = out_weight.shape[0]
    scale = 1.0 / math.sqrt(length * n_sp * n_dp)
    ext = -(-(tap_count - 1) // 16) * 16
    blocks = channels // LANES
    streams = STREAMS
    while streams > 1 and (local_rows // streams) % LANES:
        streams //= 2
    stream_rows = local_rows // streams
    plan, final = stage_plan(n_sp, stream_rows)
    full_rows = max([rows for halve, rows in plan if not halve] + [8])
    small_rows = -(-(tap_count + 2) // 8) * 8
    steps = int(math.log2(n_sp)) + int(math.log2(n_dp))
    dma = pltpu.SemaphoreType.DMA
    vmem = pltpu.VMEM
    peers = max(n_dp - 1, 1)
    spec = pl.BlockSpec(memory_space=pltpu.VMEM)
    grad_value, grad_gate, grad_weight, small = pl.pallas_call(
        functools.partial(kernel, n_sp, n_dp, plan),
        out_shape=[
            jax.ShapeDtypeStruct((length, channels), bf16),
            jax.ShapeDtypeStruct((length, channels), bf16),
            jax.ShapeDtypeStruct((local_rows, channels), bf16),
            jax.ShapeDtypeStruct((small_rows, channels), f32),
        ],
        in_specs=[spec] * 7,
        out_specs=[spec] * 4,
        scratch_shapes=[
            vmem((blocks, ext + length, LANES), f32),
            vmem((blocks, length + ext, LANES), f32),
            vmem((length, channels), f32),
            vmem((length, 1), f32),
            vmem((length, channels), bf16),
            vmem((length, channels), f32),
            vmem((n_dp, local_rows, channels), bf16),
            vmem((ext, channels), bf16),
            vmem((ext, channels), bf16),
            vmem((blocks, ext, LANES), f32),
            vmem((blocks, ext, LANES), f32),
            vmem((2, blocks, 8, LANES), f32),
            vmem((small_rows, channels), f32),
            vmem((steps, small_rows, channels), f32),
            vmem((peers, streams, stream_rows, channels), f32),
            vmem((peers, streams, stream_rows, channels), f32),
            vmem((streams, stream_rows, channels), f32),
            vmem((streams, stream_rows, channels), bf16),
            vmem((streams, stream_rows, channels), bf16),
            vmem((streams, stream_rows, channels), f32),
            vmem((streams, len(plan), full_rows, channels), f32),
            vmem((local_rows, channels), bf16),
            dma,
            dma((peers,)), dma((peers,)),
            dma((3,)), dma((3,)),
            dma((streams, peers)), dma((streams, peers)),
            dma((streams, 2 * len(plan))), dma((streams, 2 * len(plan))),
            dma((steps,)), dma((steps,)),
        ],
        compiler_params=pltpu.CompilerParams(
            collective_id=0, has_side_effects=True, vmem_limit_bytes=60 * 1024 * 1024
        ),
    )(glu_value[0], glu_gate[0], cotangent[0], conv_weight, norm_gain[None], norm_shift[None], out_weight)
    small = small * scale
    return (
        grad_value[None],
        grad_gate[None],
        grad_weight.astype(f32) * scale,
        small[:tap_count],
        small[tap_count],
        small[tap_count + 1],
    )


def solution(mesh):
    in_specs = (
        P("dp", "sp", None),
        P("dp", "sp", None),
        P("dp", "sp", None),
        P(),
        P(),
        P(),
        P("dp", None),
    )
    out_specs = (P("dp", "sp", None), P("dp", "sp", None), P("dp", None), P(), P(), P())
    return jax.shard_map(
        per_device, mesh=mesh, in_specs=in_specs, out_specs=out_specs, check_vma=False
    )
```

```python
import functools
import math

import jax
import jax.numpy as jnp
from jax import lax
from jax.experimental import pallas as pl
from jax.experimental.pallas import tpu as pltpu
from jax.sharding import PartitionSpec as P

epsilon = 1e-06
LANES = 128
STREAMS = 4
NARROW_STAGES = 3
MAX_HALVINGS = 4
SMALL_HALVINGS = 2
f32 = jnp.float32
bf16 = jnp.bfloat16


def flip(index, bit):
    size = 1 << bit
    here = (index // size) % 2
    return here, index + (1 - 2 * here) * size


def stage_plan(n_sp, rows):
    bits = int(math.log2(n_sp))
    plan = []
    for stage in range(bits):
        halve = stage < MAX_HALVINGS and rows // 2 >= 16
        plan.append((halve, rows))
        if halve:
            rows //= 2
    return plan, rows


def bit_order(n_sp, stream):
    order = list(range(int(math.log2(n_sp))))
    if stream % 2 and len(order) > 1:
        order[0], order[1] = order[1], order[0]
    return order


def kernel(
    n_sp, n_dp, plan, scale,
    value, gate, cotan, taps, gain, shift, weight,
    grad_value, grad_gate, out_weight, out_taps, out_gain, out_shift,
    gated, grads, normed, inv, act, grad_act, weights,
    halo_v, halo_g, edge_out, edge_in, sums, small, small_in, small_done,
    dp_out, dp_in, acc, narrow_out, narrow_in, wide_in, full_in, gathered,
    local_sem, w_send, w_recv, h_send, h_recv, dp_send, dp_recv, st_send, st_recv, sm_send, sm_recv,
):
    sp = lax.axis_index("sp")
    dp = lax.axis_index("dp")
    length, channels = value.shape
    tap_count = taps.shape[0]
    blocks = channels // LANES
    ext = grads.shape[1] - length
    lead = ext - (tap_count - 1)
    local_rows = weight.shape[0]
    streams, stream_rows = acc.shape[0], acc.shape[1]
    block_rows = min(64, length)
    row_blocks = length // block_rows
    sp_bits = int(math.log2(n_sp))
    dp_bits = int(math.log2(n_dp))
    later = (sp + 1) % n_sp
    prior = (sp + n_sp - 1) % n_sp

    barrier = pltpu.get_barrier_semaphore()
    partners = [{"sp": later}, {"sp": prior}]
    partners += [{"sp": flip(sp, b)[1]} for b in range(sp_bits)]
    partners += [{"dp": (dp + o) % n_dp} for o in range(1, n_dp)]
    for partner in partners:
        pl.semaphore_signal(barrier, inc=1, device_id=partner, device_id_type=pl.DeviceIdType.MESH)
    pl.semaphore_wait(barrier, len(partners))

    def remote(src, dst, send, recv, where):
        return pltpu.make_async_remote_copy(
            src_ref=src, dst_ref=dst, send_sem=send, recv_sem=recv,
            device_id=where, device_id_type=pl.DeviceIdType.MESH,
        )

    halos = [
        remote(value.at[pl.ds(length - ext, ext)], halo_v, h_send.at[0], h_recv.at[0], {"sp": later}),
        remote(gate.at[pl.ds(length - ext, ext)], halo_g, h_send.at[1], h_recv.at[1], {"sp": later}),
    ]
    for copy in halos:
        copy.start()
    own = pltpu.make_async_copy(weight, weights.at[dp], local_sem)
    own.start()
    w_copies = []
    for o in range(1, n_dp):
        w_copies.append(
            remote(weight, weights.at[dp], w_send.at[o - 1], w_recv.at[o - 1], {"dp": (dp + o) % n_dp})
        )
        w_copies[-1].start()

    def cols(b):
        return pl.ds(b * LANES, LANES)

    def gate_rows(v, g):
        return v.astype(f32) * jax.nn.sigmoid(g.astype(f32))

    def gating(i, _):
        r0 = pl.multiple_of(i * block_rows, block_rows)
        for b in range(blocks):
            gated[b, pl.ds(ext + r0, block_rows), :] = gate_rows(
                value[pl.ds(r0, block_rows), cols(b)], gate[pl.ds(r0, block_rows), cols(b)]
            )
        return 0

    lax.fori_loop(0, row_blocks, gating, 0)
    def fill_halo():
        for copy in halos:
            copy.wait()
        for b in range(blocks):
            gated[b, 0:ext, :] = jnp.where(sp > 0, gate_rows(halo_v[:, cols(b)], halo_g[:, cols(b)]), 0.0)

    def row_mean(parts):
        total = parts[0]
        for p in parts[1:]:
            total = total + p
        return jnp.sum(total, axis=-1, keepdims=True) * (1.0 / channels)

    def forward(i, _):
        r0 = pl.multiple_of(i * block_rows, block_rows)
        rows = pl.ds(r0, block_rows)
        convs = []
        for b in range(blocks):
            total = jnp.zeros((block_rows, LANES), f32)
            for j in range(tap_count):
                total = total + taps[j : j + 1, cols(b)] * gated[b, pl.ds(r0 + lead + j, block_rows), :]
            convs.append(total)
        mean = row_mean(convs)
        centred = [c - mean for c in convs]
        inv_std = lax.rsqrt(row_mean([c * c for c in centred]) + epsilon)
        inv[rows, :] = inv_std
        for b in range(blocks):
            n = centred[b] * inv_std
            normed[rows, cols(b)] = n
            pre = n * gain[:, cols(b)] + shift[:, cols(b)]
            act[rows, cols(b)] = (pre * jax.nn.sigmoid(pre)).astype(bf16)
        return 0

    lax.fori_loop(1, row_blocks, forward, 0)
    fill_halo()
    forward(0, 0)

    dp_copies = [[None] * (n_dp - 1) for _ in range(streams)]

    def product(chunk, stream):
        start = pl.multiple_of(chunk * local_rows + stream * stream_rows, LANES)
        return lax.dot_general(
            cotan[:, pl.ds(start, stream_rows)], act[...], (((0,), (0,)), ((), ())),
            preferred_element_type=f32,
        )

    def exchange(k):
        order = bit_order(n_sp, k)
        for copy in dp_copies[k]:
            copy.wait()
        for o in range(1, n_dp):
            acc[k] += dp_in[o - 1, k]
        off = 0
        final = stream_rows
        for stage, (halve, rows) in enumerate(plan):
            here, partner = flip(sp, order[stage])
            sems = st_send.at[k, stage], st_recv.at[k, stage], {"sp": partner}
            if halve:
                half = rows // 2
                final = half
                spot = pl.ds(stream_rows - rows, half)
                out = pl.ds(pl.multiple_of(off + (1 - here) * half, half), half)
                off = off + here * half
                into = pl.ds(pl.multiple_of(off, half), half)
                if stage < NARROW_STAGES:
                    narrow_out[k, spot, :] = acc[k, out, :].astype(bf16)
                    copy = remote(narrow_out.at[k, spot], narrow_in.at[k, spot], *sems)
                    landed = narrow_in
                else:
                    copy = remote(acc.at[k, out], wide_in.at[k, spot], *sems)
                    landed = wide_in
                copy.start()
                yield
                copy.wait()
                acc[k, into, :] += landed[k, spot, :].astype(f32)
            else:
                into = pl.ds(pl.multiple_of(off, rows), rows)
                copy = remote(acc.at[k, into], full_in.at[k, stage], *sems)
                copy.start()
                yield
                copy.wait()
                acc[k, into, :] += full_in[k, stage]
        spot = pl.ds(pl.multiple_of(off, final), final)
        wide = pl.ds(pl.multiple_of(k * stream_rows + off, final), final)
        gathered[wide, :] = acc[k, spot, :].astype(bf16)
        for stage in reversed(range(len(plan))):
            halve, rows = plan[stage]
            if not halve:
                continue
            half = rows // 2
            here, partner = flip(sp, order[stage])
            spot = pl.ds(pl.multiple_of(k * stream_rows + off, half), half)
            back = len(plan) + stage
            copy = remote(
                gathered.at[spot], gathered.at[spot],
                st_send.at[k, back], st_recv.at[k, back], {"sp": partner},
            )
            copy.start()
            yield
            copy.wait()
            off = off - here * half
        out_weight[pl.ds(k * stream_rows, stream_rows), :] = gathered[pl.ds(k * stream_rows, stream_rows), :]

    def combine():
        axes = [("dp", dp, b) for b in range(dp_bits)] + [("sp", sp, b) for b in range(sp_bits)]
        low, count = 0, blocks
        halved = []
        for step, (name, index, b) in enumerate(axes):
            here, partner = flip(index, b)
            sems = sm_send.at[step], sm_recv.at[step], {name: partner}
            if step < SMALL_HALVINGS and count > 1:
                count //= 2
                src = small.at[pl.ds(low + (1 - here) * count, count)]
                low = low + here * count
                halved.append((here, count, name, partner))
            else:
                src = small.at[pl.ds(low, count)]
            copy = remote(src, small_in.at[step, pl.ds(0, count)], *sems)
            copy.start()
            yield
            copy.wait()
            small[pl.ds(low, count)] += small_in[step, 0:count]
        small_done[pl.ds(low, count)] = small[pl.ds(low, count)]
        for back, (here, count, name, partner) in enumerate(reversed(halved)):
            slot = len(axes) + back
            span = small_done.at[pl.ds(low, count)]
            copy = remote(span, span, sm_send.at[slot], sm_recv.at[slot], {name: partner})
            copy.start()
            yield
            copy.wait()
            low = low - here * count
        for b in range(blocks):
            out_taps[:, cols(b)] = small_done[b, 0:tap_count, :] * scale
            out_gain[:, cols(b)] = small_done[b, tap_count : tap_count + 1, :] * scale
            out_shift[:, cols(b)] = small_done[b, tap_count + 1 : tap_count + 2, :] * scale

    flows = [exchange(k) for k in range(streams)]

    def advance():
        for flow in list(flows):
            if next(flow, "end") == "end":
                flows.remove(flow)

    for k in range(streams):
        for o in range(1, n_dp):
            peer = (dp + o) % n_dp
            dp_out[o - 1, k] = product(peer, k)
            copy = remote(
                dp_out.at[o - 1, k], dp_in.at[o - 1, k],
                dp_send.at[k, o - 1], dp_recv.at[k, o - 1], {"dp": peer},
            )
            copy.start()
            dp_copies[k][o - 1] = copy
        acc[k] = product(dp, k)
        if k:
            next(flows[k - 1])
    next(flows[streams - 1])

    for copy in w_copies:
        copy.wait()
    own.wait()
    total = None
    for d in range(n_dp):
        part = jnp.dot(cotan[:, d * local_rows : (d + 1) * local_rows], weights[d], preferred_element_type=f32)
        total = part if total is None else total + part
    grad_act[...] = total
    advance()
    sums[...] = jnp.zeros_like(sums)

    def backward(i):
        r0 = pl.multiple_of(i * block_rows, block_rows)
        rows = pl.ds(r0, block_rows)
        inv_std = inv[rows, :]
        normal, grad_normal = [], []
        for b in range(blocks):
            n = normed[rows, cols(b)]
            pre = n * gain[:, cols(b)] + shift[:, cols(b)]
            s = jax.nn.sigmoid(pre)
            grad_pre = grad_act[rows, cols(b)] * s * (1.0 + pre * (1.0 - s))
            sums[0, b] += jnp.sum((grad_pre * n).reshape(block_rows // 8, 8, LANES), axis=0)
            sums[1, b] += jnp.sum(grad_pre.reshape(block_rows // 8, 8, LANES), axis=0)
            normal.append(n)
            grad_normal.append(grad_pre * gain[:, cols(b)])
        first = row_mean(grad_normal)
        second = row_mean([g * n for g, n in zip(grad_normal, normal)])
        for b in range(blocks):
            grads[b, rows, :] = inv_std * (grad_normal[b] - first - normal[b] * second)

    backward(0)
    edge_out[...] = grads[:, 0:ext, :]
    edge = remote(edge_out, edge_in, h_send.at[2], h_recv.at[2], {"sp": prior})
    edge.start()

    def backward_loop(i, _):
        backward(i)
        return 0

    lax.fori_loop(1, row_blocks, backward_loop, 0)
    advance()

    small[...] = jnp.zeros_like(small)
    for b in range(blocks):

        def tap_rows(i, carry):
            r0 = pl.multiple_of(i * 8, 8)
            g = grads[b, pl.ds(r0, 8), :]
            return tuple(c + g * gated[b, pl.ds(r0 + lead + j, 8), :] for j, c in enumerate(carry))

        found = lax.fori_loop(
            0, length // 8, tap_rows, tuple(jnp.zeros((8, LANES), f32) for _ in range(tap_count))
        )
        for j in range(tap_count):
            small[b, j : j + 1, :] = jnp.sum(found[j], axis=0, keepdims=True)
        for row in range(2):
            small[b, tap_count + row : tap_count + row + 1, :] = jnp.sum(sums[row, b], axis=0, keepdims=True)
        if b % 2:
            advance()
    flows.insert(0, combine())
    edge.wait()
    for b in range(blocks):
        grads[b, pl.ds(length, ext), :] = jnp.where(sp < n_sp - 1, edge_in[b], 0.0)
    advance()

    def final_rows(i, _):
        r0 = pl.multiple_of(i * block_rows, block_rows)
        rows = pl.ds(r0, block_rows)
        for b in range(blocks):
            total = jnp.zeros((block_rows, LANES), f32)
            for j in range(tap_count):
                total = total + taps[j : j + 1, cols(b)] * grads[b, pl.ds(r0 + tap_count - 1 - j, block_rows), :]
            s = jax.nn.sigmoid(gate[rows, cols(b)].astype(f32))
            grad_value[rows, cols(b)] = (total * s).astype(bf16)
            grad_gate[rows, cols(b)] = (total * value[rows, cols(b)].astype(f32) * s * (1.0 - s)).astype(bf16)
        return 0

    pieces = math.gcd(row_blocks, 4)
    step = row_blocks // pieces
    for piece in range(pieces):
        lax.fori_loop(piece * step, (piece + 1) * step, final_rows, 0)
        advance()
    while flows:
        advance()


def per_device(glu_value, glu_gate, cotangent, conv_weight, norm_gain, norm_shift, out_weight):
    n_sp, n_dp = lax.axis_size("sp"), lax.axis_size("dp")
    length, channels = glu_value.shape[1:]
    features = cotangent.shape[2]
    tap_count = conv_weight.shape[0]
    local_rows = out_weight.shape[0]
    scale = 1.0 / math.sqrt(length * n_sp * n_dp)
    ext = -(-(tap_count - 1) // 16) * 16
    blocks = channels // LANES
    streams = STREAMS
    while streams > 1 and (local_rows // streams) % LANES:
        streams //= 2
    stream_rows = local_rows // streams
    plan, final = stage_plan(n_sp, stream_rows)
    full_rows = max([rows for halve, rows in plan if not halve] + [8])
    small_rows = -(-(tap_count + 2) // 8) * 8
    steps = int(math.log2(n_sp)) + int(math.log2(n_dp))
    dma = pltpu.SemaphoreType.DMA
    vmem = pltpu.VMEM
    peers = max(n_dp - 1, 1)
    spec = pl.BlockSpec(memory_space=pltpu.VMEM)
    grad_value, grad_gate, grad_weight, grad_conv, grad_gain, grad_shift = pl.pallas_call(
        functools.partial(kernel, n_sp, n_dp, plan, scale),
        out_shape=[
            jax.ShapeDtypeStruct((length, channels), bf16),
            jax.ShapeDtypeStruct((length, channels), bf16),
            jax.ShapeDtypeStruct((local_rows, channels), bf16),
            jax.ShapeDtypeStruct((tap_count, channels), f32),
            jax.ShapeDtypeStruct((1, channels), f32),
            jax.ShapeDtypeStruct((1, channels), f32),
        ],
        in_specs=[spec] * 7,
        out_specs=[spec] * 6,
        scratch_shapes=[
            vmem((blocks, ext + length, LANES), f32),
            vmem((blocks, length + ext, LANES), f32),
            vmem((length, channels), f32),
            vmem((length, 1), f32),
            vmem((length, channels), bf16),
            vmem((length, channels), f32),
            vmem((n_dp, local_rows, channels), bf16),
            vmem((ext, channels), bf16),
            vmem((ext, channels), bf16),
            vmem((blocks, ext, LANES), f32),
            vmem((blocks, ext, LANES), f32),
            vmem((2, blocks, 8, LANES), f32),
            vmem((blocks, small_rows, LANES), f32),
            vmem((steps, blocks, small_rows, LANES), f32),
            vmem((blocks, small_rows, LANES), f32),
            vmem((peers, streams, stream_rows, channels), f32),
            vmem((peers, streams, stream_rows, channels), f32),
            vmem((streams, stream_rows, channels), f32),
            vmem((streams, stream_rows, channels), bf16),
            vmem((streams, stream_rows, channels), bf16),
            vmem((streams, stream_rows, channels), f32),
            vmem((streams, len(plan), full_rows, channels), f32),
            vmem((local_rows, channels), bf16),
            dma,
            dma((peers,)), dma((peers,)),
            dma((3,)), dma((3,)),
            dma((streams, peers)), dma((streams, peers)),
            dma((streams, 2 * len(plan))), dma((streams, 2 * len(plan))),
            dma((2 * steps,)), dma((2 * steps,)),
        ],
        compiler_params=pltpu.CompilerParams(
            collective_id=0, has_side_effects=True, vmem_limit_bytes=60 * 1024 * 1024
        ),
    )(glu_value[0], glu_gate[0], cotangent[0], conv_weight, norm_gain[None], norm_shift[None], out_weight)
    return (
        grad_value[None],
        grad_gate[None],
        grad_weight.astype(f32) * scale,
        grad_conv,
        grad_gain[0],
        grad_shift[0],
    )


def solution(mesh):
    in_specs = (
        P("dp", "sp", None),
        P("dp", "sp", None),
        P("dp", "sp", None),
        P(),
        P(),
        P(),
        P("dp", None),
    )
    out_specs = (P("dp", "sp", None), P("dp", "sp", None), P("dp", None), P(), P(), P())
    return jax.shard_map(
        per_device, mesh=mesh, in_specs=in_specs, out_specs=out_specs, check_vma=False
    )
```

```python
import functools
import math

import jax
import jax.numpy as jnp
from jax import lax
from jax.experimental import pallas as pl
from jax.experimental.pallas import tpu as pltpu
from jax.sharding import PartitionSpec as P

epsilon = 1e-06
LANES = 128
STREAMS = 4
NARROW_STAGES = 3
MAX_HALVINGS = 4
SMALL_HALVINGS = 1
f32 = jnp.float32
bf16 = jnp.bfloat16


def flip(index, bit):
    size = 1 << bit
    here = (index // size) % 2
    return here, index + (1 - 2 * here) * size


def stage_plan(n_sp, rows):
    bits = int(math.log2(n_sp))
    plan = []
    for stage in range(bits):
        halve = stage < MAX_HALVINGS and rows // 2 >= 16
        plan.append((halve, rows))
        if halve:
            rows //= 2
    return plan, rows


def bit_order(n_sp, stream):
    order = list(range(int(math.log2(n_sp))))
    if stream % 2 and len(order) > 1:
        order[0], order[1] = order[1], order[0]
    return order


def kernel(
    n_sp, n_dp, plan, scale,
    value, gate, cotan, taps, gain, shift, weight,
    grad_value, grad_gate, out_weight, out_taps, out_gain, out_shift,
    gated, grads, normed, inv, act, grad_act, weights,
    halo_v, halo_g, edge_out, edge_in, sums, small, small_in, small_done,
    dp_out, dp_in, acc, narrow_out, narrow_in, wide_in, full_in, gathered,
    local_sem, w_send, w_recv, h_send, h_recv, dp_send, dp_recv, st_send, st_recv, sm_send, sm_recv,
):
    sp = lax.axis_index("sp")
    dp = lax.axis_index("dp")
    length, channels = value.shape
    tap_count = taps.shape[0]
    blocks = channels // LANES
    ext = grads.shape[1] - length
    lead = ext - (tap_count - 1)
    local_rows = weight.shape[0]
    streams, stream_rows = acc.shape[0], acc.shape[1]
    block_rows = min(64, length)
    row_blocks = length // block_rows
    sp_bits = int(math.log2(n_sp))
    dp_bits = int(math.log2(n_dp))
    later = (sp + 1) % n_sp
    prior = (sp + n_sp - 1) % n_sp

    barrier = pltpu.get_barrier_semaphore()
    partners = [{"sp": later}, {"sp": prior}]
    partners += [{"sp": flip(sp, b)[1]} for b in range(sp_bits)]
    partners += [{"dp": (dp + o) % n_dp} for o in range(1, n_dp)]
    for partner in partners:
        pl.semaphore_signal(barrier, inc=1, device_id=partner, device_id_type=pl.DeviceIdType.MESH)
    pl.semaphore_wait(barrier, len(partners))

    def remote(src, dst, send, recv, where):
        return pltpu.make_async_remote_copy(
            src_ref=src, dst_ref=dst, send_sem=send, recv_sem=recv,
            device_id=where, device_id_type=pl.DeviceIdType.MESH,
        )

    halos = [
        remote(value.at[pl.ds(length - ext, ext)], halo_v, h_send.at[0], h_recv.at[0], {"sp": later}),
        remote(gate.at[pl.ds(length - ext, ext)], halo_g, h_send.at[1], h_recv.at[1], {"sp": later}),
    ]
    for copy in halos:
        copy.start()
    own = pltpu.make_async_copy(weight, weights.at[dp], local_sem)
    own.start()
    w_copies = []
    for o in range(1, n_dp):
        w_copies.append(
            remote(weight, weights.at[dp], w_send.at[o - 1], w_recv.at[o - 1], {"dp": (dp + o) % n_dp})
        )
        w_copies[-1].start()

    def cols(b):
        return pl.ds(b * LANES, LANES)

    def gate_rows(v, g):
        return v.astype(f32) * jax.nn.sigmoid(g.astype(f32))

    def gating(i, _):
        r0 = pl.multiple_of(i * block_rows, block_rows)
        for b in range(blocks):
            gated[b, pl.ds(ext + r0, block_rows), :] = gate_rows(
                value[pl.ds(r0, block_rows), cols(b)], gate[pl.ds(r0, block_rows), cols(b)]
            )
        return 0

    lax.fori_loop(0, row_blocks, gating, 0)
    def fill_halo():
        for copy in halos:
            copy.wait()
        for b in range(blocks):
            gated[b, 0:ext, :] = jnp.where(sp > 0, gate_rows(halo_v[:, cols(b)], halo_g[:, cols(b)]), 0.0)

    def row_mean(parts):
        total = parts[0]
        for p in parts[1:]:
            total = total + p
        return jnp.sum(total, axis=-1, keepdims=True) * (1.0 / channels)

    def forward(i, _):
        r0 = pl.multiple_of(i * block_rows, block_rows)
        rows = pl.ds(r0, block_rows)
        convs = []
        for b in range(blocks):
            total = jnp.zeros((block_rows, LANES), f32)
            for j in range(tap_count):
                total = total + taps[j : j + 1, cols(b)] * gated[b, pl.ds(r0 + lead + j, block_rows), :]
            convs.append(total)
        mean = row_mean(convs)
        centred = [c - mean for c in convs]
        inv_std = lax.rsqrt(row_mean([c * c for c in centred]) + epsilon)
        inv[rows, :] = inv_std
        for b in range(blocks):
            n = centred[b] * inv_std
            normed[rows, cols(b)] = n
            pre = n * gain[:, cols(b)] + shift[:, cols(b)]
            act[rows, cols(b)] = (pre * jax.nn.sigmoid(pre)).astype(bf16)
        return 0

    lax.fori_loop(1, row_blocks, forward, 0)
    fill_halo()
    forward(0, 0)

    dp_copies = [[None] * (n_dp - 1) for _ in range(streams)]

    def product(chunk, stream):
        start = pl.multiple_of(chunk * local_rows + stream * stream_rows, LANES)
        return lax.dot_general(
            cotan[:, pl.ds(start, stream_rows)], act[...], (((0,), (0,)), ((), ())),
            preferred_element_type=f32,
        )

    def exchange(k):
        order = bit_order(n_sp, k)
        for copy in dp_copies[k]:
            copy.wait()
        for o in range(1, n_dp):
            acc[k] += dp_in[o - 1, k]
        off = 0
        final = stream_rows
        for stage, (halve, rows) in enumerate(plan):
            here, partner = flip(sp, order[stage])
            sems = st_send.at[k, stage], st_recv.at[k, stage], {"sp": partner}
            if halve:
                half = rows // 2
                final = half
                spot = pl.ds(stream_rows - rows, half)
                out = pl.ds(pl.multiple_of(off + (1 - here) * half, half), half)
                off = off + here * half
                into = pl.ds(pl.multiple_of(off, half), half)
                if stage < NARROW_STAGES:
                    narrow_out[k, spot, :] = acc[k, out, :].astype(bf16)
                    copy = remote(narrow_out.at[k, spot], narrow_in.at[k, spot], *sems)
                    landed = narrow_in
                else:
                    copy = remote(acc.at[k, out], wide_in.at[k, spot], *sems)
                    landed = wide_in
                copy.start()
                yield
                copy.wait()
                acc[k, into, :] += landed[k, spot, :].astype(f32)
            else:
                into = pl.ds(pl.multiple_of(off, rows), rows)
                copy = remote(acc.at[k, into], full_in.at[k, stage], *sems)
                copy.start()
                yield
                copy.wait()
                acc[k, into, :] += full_in[k, stage]
        spot = pl.ds(pl.multiple_of(off, final), final)
        wide = pl.ds(pl.multiple_of(k * stream_rows + off, final), final)
        gathered[wide, :] = acc[k, spot, :].astype(bf16)
        for stage in reversed(range(len(plan))):
            halve, rows = plan[stage]
            if not halve:
                continue
            half = rows // 2
            here, partner = flip(sp, order[stage])
            spot = pl.ds(pl.multiple_of(k * stream_rows + off, half), half)
            back = len(plan) + stage
            copy = remote(
                gathered.at[spot], gathered.at[spot],
                st_send.at[k, back], st_recv.at[k, back], {"sp": partner},
            )
            copy.start()
            yield
            copy.wait()
            off = off - here * half
        out_weight[pl.ds(k * stream_rows, stream_rows), :] = gathered[pl.ds(k * stream_rows, stream_rows), :]

    def combine():
        axes = [("dp", dp, b) for b in range(dp_bits)] + [("sp", sp, b) for b in range(sp_bits)]
        low, count = 0, blocks
        halved = []
        for step, (name, index, b) in enumerate(axes):
            here, partner = flip(index, b)
            sems = sm_send.at[step], sm_recv.at[step], {name: partner}
            if step < SMALL_HALVINGS and count > 1:
                count //= 2
                src = small.at[pl.ds(low + (1 - here) * count, count)]
                low = low + here * count
                halved.append((here, count, name, partner))
            else:
                src = small.at[pl.ds(low, count)]
            copy = remote(src, small_in.at[step, pl.ds(0, count)], *sems)
            copy.start()
            yield
            copy.wait()
            small[pl.ds(low, count)] += small_in[step, 0:count]
        small_done[pl.ds(low, count)] = small[pl.ds(low, count)]
        for back, (here, count, name, partner) in enumerate(reversed(halved)):
            slot = len(axes) + back
            span = small_done.at[pl.ds(low, count)]
            copy = remote(span, span, sm_send.at[slot], sm_recv.at[slot], {name: partner})
            copy.start()
            yield
            copy.wait()
            low = low - here * count
        for b in range(blocks):
            out_taps[:, cols(b)] = small_done[b, 0:tap_count, :] * scale
            out_gain[:, cols(b)] = small_done[b, tap_count : tap_count + 1, :] * scale
            out_shift[:, cols(b)] = small_done[b, tap_count + 1 : tap_count + 2, :] * scale

    flows = [exchange(k) for k in range(streams)]

    def advance():
        for flow in list(flows):
            if next(flow, "end") == "end":
                flows.remove(flow)

    for k in range(streams):
        for o in range(1, n_dp):
            peer = (dp + o) % n_dp
            dp_out[o - 1, k] = product(peer, k)
            copy = remote(
                dp_out.at[o - 1, k], dp_in.at[o - 1, k],
                dp_send.at[k, o - 1], dp_recv.at[k, o - 1], {"dp": peer},
            )
            copy.start()
            dp_copies[k][o - 1] = copy
        acc[k] = product(dp, k)

    for copy in w_copies:
        copy.wait()
    own.wait()
    total = None
    for d in range(n_dp):
        part = jnp.dot(cotan[:, d * local_rows : (d + 1) * local_rows], weights[d], preferred_element_type=f32)
        total = part if total is None else total + part
    grad_act[...] = total
    advance()
    sums[...] = jnp.zeros_like(sums)

    def backward(i):
        r0 = pl.multiple_of(i * block_rows, block_rows)
        rows = pl.ds(r0, block_rows)
        inv_std = inv[rows, :]
        normal, grad_normal = [], []
        for b in range(blocks):
            n = normed[rows, cols(b)]
            pre = n * gain[:, cols(b)] + shift[:, cols(b)]
            s = jax.nn.sigmoid(pre)
            grad_pre = grad_act[rows, cols(b)] * s * (1.0 + pre * (1.0 - s))
            sums[0, b] += jnp.sum((grad_pre * n).reshape(block_rows // 8, 8, LANES), axis=0)
            sums[1, b] += jnp.sum(grad_pre.reshape(block_rows // 8, 8, LANES), axis=0)
            normal.append(n)
            grad_normal.append(grad_pre * gain[:, cols(b)])
        first = row_mean(grad_normal)
        second = row_mean([g * n for g, n in zip(grad_normal, normal)])
        for b in range(blocks):
            grads[b, rows, :] = inv_std * (grad_normal[b] - first - normal[b] * second)

    backward(0)
    edge_out[...] = grads[:, 0:ext, :]
    edge = remote(edge_out, edge_in, h_send.at[2], h_recv.at[2], {"sp": prior})
    edge.start()

    def backward_loop(i, _):
        backward(i)
        return 0

    lax.fori_loop(1, row_blocks, backward_loop, 0)

    small[...] = jnp.zeros_like(small)
    for b in range(blocks):

        def tap_rows(i, carry):
            r0 = pl.multiple_of(i * 8, 8)
            g = grads[b, pl.ds(r0, 8), :]
            return tuple(c + g * gated[b, pl.ds(r0 + lead + j, 8), :] for j, c in enumerate(carry))

        found = lax.fori_loop(
            0, length // 8, tap_rows, tuple(jnp.zeros((8, LANES), f32) for _ in range(tap_count))
        )
        for j in range(tap_count):
            small[b, j : j + 1, :] = jnp.sum(found[j], axis=0, keepdims=True)
        for row in range(2):
            small[b, tap_count + row : tap_count + row + 1, :] = jnp.sum(sums[row, b], axis=0, keepdims=True)
    flows.insert(0, combine())
    edge.wait()
    for b in range(blocks):
        grads[b, pl.ds(length, ext), :] = jnp.where(sp < n_sp - 1, edge_in[b], 0.0)
    advance()

    def final_rows(i, _):
        r0 = pl.multiple_of(i * block_rows, block_rows)
        rows = pl.ds(r0, block_rows)
        for b in range(blocks):
            total = jnp.zeros((block_rows, LANES), f32)
            for j in range(tap_count):
                total = total + taps[j : j + 1, cols(b)] * grads[b, pl.ds(r0 + tap_count - 1 - j, block_rows), :]
            s = jax.nn.sigmoid(gate[rows, cols(b)].astype(f32))
            grad_value[rows, cols(b)] = (total * s).astype(bf16)
            grad_gate[rows, cols(b)] = (total * value[rows, cols(b)].astype(f32) * s * (1.0 - s)).astype(bf16)
        return 0

    pieces = math.gcd(row_blocks, 4)
    step = row_blocks // pieces
    for piece in range(pieces):
        lax.fori_loop(piece * step, (piece + 1) * step, final_rows, 0)
        advance()
    while flows:
        advance()


def per_device(glu_value, glu_gate, cotangent, conv_weight, norm_gain, norm_shift, out_weight):
    n_sp, n_dp = lax.axis_size("sp"), lax.axis_size("dp")
    length, channels = glu_value.shape[1:]
    features = cotangent.shape[2]
    tap_count = conv_weight.shape[0]
    local_rows = out_weight.shape[0]
    scale = 1.0 / math.sqrt(length * n_sp * n_dp)
    ext = -(-(tap_count - 1) // 16) * 16
    blocks = channels // LANES
    streams = STREAMS
    while streams > 1 and (local_rows // streams) % LANES:
        streams //= 2
    stream_rows = local_rows // streams
    plan, final = stage_plan(n_sp, stream_rows)
    full_rows = max([rows for halve, rows in plan if not halve] + [8])
    small_rows = -(-(tap_count + 2) // 8) * 8
    steps = int(math.log2(n_sp)) + int(math.log2(n_dp))
    dma = pltpu.SemaphoreType.DMA
    vmem = pltpu.VMEM
    peers = max(n_dp - 1, 1)
    spec = pl.BlockSpec(memory_space=pltpu.VMEM)
    grad_value, grad_gate, grad_weight, grad_conv, grad_gain, grad_shift = pl.pallas_call(
        functools.partial(kernel, n_sp, n_dp, plan, scale),
        out_shape=[
            jax.ShapeDtypeStruct((length, channels), bf16),
            jax.ShapeDtypeStruct((length, channels), bf16),
            jax.ShapeDtypeStruct((local_rows, channels), bf16),
            jax.ShapeDtypeStruct((tap_count, channels), f32),
            jax.ShapeDtypeStruct((1, channels), f32),
            jax.ShapeDtypeStruct((1, channels), f32),
        ],
        in_specs=[spec] * 7,
        out_specs=[spec] * 6,
        scratch_shapes=[
            vmem((blocks, ext + length, LANES), f32),
            vmem((blocks, length + ext, LANES), f32),
            vmem((length, channels), f32),
            vmem((length, 1), f32),
            vmem((length, channels), bf16),
            vmem((length, channels), f32),
            vmem((n_dp, local_rows, channels), bf16),
            vmem((ext, channels), bf16),
            vmem((ext, channels), bf16),
            vmem((blocks, ext, LANES), f32),
            vmem((blocks, ext, LANES), f32),
            vmem((2, blocks, 8, LANES), f32),
            vmem((blocks, small_rows, LANES), f32),
            vmem((steps, blocks, small_rows, LANES), f32),
            vmem((blocks, small_rows, LANES), f32),
            vmem((peers, streams, stream_rows, channels), f32),
            vmem((peers, streams, stream_rows, channels), f32),
            vmem((streams, stream_rows, channels), f32),
            vmem((streams, stream_rows, channels), bf16),
            vmem((streams, stream_rows, channels), bf16),
            vmem((streams, stream_rows, channels), f32),
            vmem((streams, len(plan), full_rows, channels), f32),
            vmem((local_rows, channels), bf16),
            dma,
            dma((peers,)), dma((peers,)),
            dma((3,)), dma((3,)),
            dma((streams, peers)), dma((streams, peers)),
            dma((streams, 2 * len(plan))), dma((streams, 2 * len(plan))),
            dma((2 * steps,)), dma((2 * steps,)),
        ],
        compiler_params=pltpu.CompilerParams(
            collective_id=0, has_side_effects=True, vmem_limit_bytes=60 * 1024 * 1024
        ),
    )(glu_value[0], glu_gate[0], cotangent[0], conv_weight, norm_gain[None], norm_shift[None], out_weight)
    return (
        grad_value[None],
        grad_gate[None],
        grad_weight.astype(f32) * scale,
        grad_conv,
        grad_gain[0],
        grad_shift[0],
    )


def solution(mesh):
    in_specs = (
        P("dp", "sp", None),
        P("dp", "sp", None),
        P("dp", "sp", None),
        P(),
        P(),
        P(),
        P("dp", None),
    )
    out_specs = (P("dp", "sp", None), P("dp", "sp", None), P("dp", None), P(), P(), P())
    return jax.shard_map(
        per_device, mesh=mesh, in_specs=in_specs, out_specs=out_specs, check_vma=False
    )
```

```python
import functools
import math

import jax
import jax.numpy as jnp
from jax import lax
from jax.experimental import pallas as pl
from jax.experimental.pallas import tpu as pltpu
from jax.sharding import PartitionSpec as P

epsilon = 1e-06
LANES = 128
STREAMS = 4
NARROW_STAGES = 3
MAX_HALVINGS = 4
SMALL_HALVINGS = 1
f32 = jnp.float32
bf16 = jnp.bfloat16


def flip(index, bit):
    size = 1 << bit
    here = (index // size) % 2
    return here, index + (1 - 2 * here) * size


def stage_plan(n_sp, rows):
    bits = int(math.log2(n_sp))
    plan = []
    for stage in range(bits):
        halve = stage < MAX_HALVINGS and rows // 2 >= 16
        plan.append((halve, rows))
        if halve:
            rows //= 2
    return plan, rows


def bit_order(n_sp, stream):
    order = list(range(int(math.log2(n_sp))))
    if stream % 2 and len(order) > 1:
        order[0], order[1] = order[1], order[0]
    return order


def kernel(
    n_sp, n_dp, plan, scale,
    value, gate, cotan, taps, gain, shift, weight,
    grad_value, grad_gate, out_weight, out_taps, out_gain, out_shift,
    gated, grads, normed, inv, act, grad_act, weights,
    halo_v, halo_g, edge_out, edge_in, sums, small, small_in, small_done,
    dp_out, dp_in, acc, narrow_out, narrow_in, wide_in, full_in, gathered,
    local_sem, w_send, w_recv, h_send, h_recv, dp_send, dp_recv, st_send, st_recv, sm_send, sm_recv,
):
    sp = lax.axis_index("sp")
    dp = lax.axis_index("dp")
    length, channels = value.shape
    tap_count = taps.shape[0]
    blocks = channels // LANES
    ext = grads.shape[1] - length
    lead = ext - (tap_count - 1)
    local_rows = weight.shape[0]
    streams, stream_rows = acc.shape[0], acc.shape[1]
    block_rows = min(64, length)
    row_blocks = length // block_rows
    sp_bits = int(math.log2(n_sp))
    dp_bits = int(math.log2(n_dp))
    later = (sp + 1) % n_sp
    prior = (sp + n_sp - 1) % n_sp

    barrier = pltpu.get_barrier_semaphore()
    partners = [{"sp": later}, {"sp": prior}]
    partners += [{"sp": flip(sp, b)[1]} for b in range(sp_bits)]
    partners += [{"dp": (dp + o) % n_dp} for o in range(1, n_dp)]
    for partner in partners:
        pl.semaphore_signal(barrier, inc=1, device_id=partner, device_id_type=pl.DeviceIdType.MESH)
    pl.semaphore_wait(barrier, len(partners))

    def remote(src, dst, send, recv, where):
        return pltpu.make_async_remote_copy(
            src_ref=src, dst_ref=dst, send_sem=send, recv_sem=recv,
            device_id=where, device_id_type=pl.DeviceIdType.MESH,
        )

    halos = [
        remote(value.at[pl.ds(length - ext, ext)], halo_v, h_send.at[0], h_recv.at[0], {"sp": later}),
        remote(gate.at[pl.ds(length - ext, ext)], halo_g, h_send.at[1], h_recv.at[1], {"sp": later}),
    ]
    for copy in halos:
        copy.start()
    own = pltpu.make_async_copy(weight, weights.at[dp], local_sem)
    own.start()
    w_copies = []
    for o in range(1, n_dp):
        w_copies.append(
            remote(weight, weights.at[dp], w_send.at[o - 1], w_recv.at[o - 1], {"dp": (dp + o) % n_dp})
        )
        w_copies[-1].start()

    def cols(b):
        return pl.ds(b * LANES, LANES)

    def gate_rows(v, g):
        return v.astype(f32) * jax.nn.sigmoid(g.astype(f32))

    def gating(i, _):
        r0 = pl.multiple_of(i * block_rows, block_rows)
        for b in range(blocks):
            gated[b, pl.ds(ext + r0, block_rows), :] = gate_rows(
                value[pl.ds(r0, block_rows), cols(b)], gate[pl.ds(r0, block_rows), cols(b)]
            )
        return 0

    lax.fori_loop(0, row_blocks, gating, 0)
    def fill_halo():
        for copy in halos:
            copy.wait()
        for b in range(blocks):
            gated[b, 0:ext, :] = jnp.where(sp > 0, gate_rows(halo_v[:, cols(b)], halo_g[:, cols(b)]), 0.0)

    def row_mean(parts):
        total = parts[0]
        for p in parts[1:]:
            total = total + p
        return jnp.sum(total, axis=-1, keepdims=True) * (1.0 / channels)

    def forward(i, _):
        r0 = pl.multiple_of(i * block_rows, block_rows)
        rows = pl.ds(r0, block_rows)
        convs = []
        for b in range(blocks):
            total = jnp.zeros((block_rows, LANES), f32)
            for j in range(tap_count):
                total = total + taps[j : j + 1, cols(b)] * gated[b, pl.ds(r0 + lead + j, block_rows), :]
            convs.append(total)
        mean = row_mean(convs)
        centred = [c - mean for c in convs]
        inv_std = lax.rsqrt(row_mean([c * c for c in centred]) + epsilon)
        inv[rows, :] = inv_std
        for b in range(blocks):
            n = centred[b] * inv_std
            normed[rows, cols(b)] = n
            pre = n * gain[:, cols(b)] + shift[:, cols(b)]
            act[rows, cols(b)] = (pre * jax.nn.sigmoid(pre)).astype(bf16)
        return 0

    lax.fori_loop(1, row_blocks, forward, 0)
    fill_halo()
    forward(0, 0)

    dp_copies = [[None] * (n_dp - 1) for _ in range(streams)]

    def product(chunk, stream):
        start = pl.multiple_of(chunk * local_rows + stream * stream_rows, LANES)
        return lax.dot_general(
            cotan[:, pl.ds(start, stream_rows)], act[...], (((0,), (0,)), ((), ())),
            preferred_element_type=f32,
        )

    def exchange(k):
        order = bit_order(n_sp, k)
        for copy in dp_copies[k]:
            copy.wait()
        for o in range(1, n_dp):
            acc[k] += dp_in[o - 1, k]
        off = 0
        final = stream_rows
        for stage, (halve, rows) in enumerate(plan):
            here, partner = flip(sp, order[stage])
            sems = st_send.at[k, stage], st_recv.at[k, stage], {"sp": partner}
            if halve:
                half = rows // 2
                final = half
                spot = pl.ds(stream_rows - rows, half)
                out = pl.ds(pl.multiple_of(off + (1 - here) * half, half), half)
                off = off + here * half
                into = pl.ds(pl.multiple_of(off, half), half)
                if stage < NARROW_STAGES:
                    narrow_out[k, spot, :] = acc[k, out, :].astype(bf16)
                    copy = remote(narrow_out.at[k, spot], narrow_in.at[k, spot], *sems)
                    landed = narrow_in
                else:
                    copy = remote(acc.at[k, out], wide_in.at[k, spot], *sems)
                    landed = wide_in
                copy.start()
                yield
                copy.wait()
                acc[k, into, :] += landed[k, spot, :].astype(f32)
            else:
                into = pl.ds(pl.multiple_of(off, rows), rows)
                copy = remote(acc.at[k, into], full_in.at[k, stage], *sems)
                copy.start()
                yield
                copy.wait()
                acc[k, into, :] += full_in[k, stage]
        spot = pl.ds(pl.multiple_of(off, final), final)
        wide = pl.ds(pl.multiple_of(k * stream_rows + off, final), final)
        gathered[wide, :] = acc[k, spot, :].astype(bf16)
        for stage in reversed(range(len(plan))):
            halve, rows = plan[stage]
            if not halve:
                continue
            half = rows // 2
            here, partner = flip(sp, order[stage])
            spot = pl.ds(pl.multiple_of(k * stream_rows + off, half), half)
            back = len(plan) + stage
            copy = remote(
                gathered.at[spot], gathered.at[spot],
                st_send.at[k, back], st_recv.at[k, back], {"sp": partner},
            )
            copy.start()
            yield
            copy.wait()
            off = off - here * half
        out_weight[pl.ds(k * stream_rows, stream_rows), :] = gathered[pl.ds(k * stream_rows, stream_rows), :]

    def combine():
        axes = [("dp", dp, b) for b in range(dp_bits)] + [("sp", sp, b) for b in range(sp_bits)]
        low, count = 0, blocks
        halved = []
        for step, (name, index, b) in enumerate(axes):
            here, partner = flip(index, b)
            sems = sm_send.at[step], sm_recv.at[step], {name: partner}
            if step < SMALL_HALVINGS and count > 1:
                count //= 2
                src = small.at[pl.ds(low + (1 - here) * count, count)]
                low = low + here * count
                halved.append((here, count, name, partner))
            else:
                src = small.at[pl.ds(low, count)]
            copy = remote(src, small_in.at[step, pl.ds(0, count)], *sems)
            copy.start()
            yield
            copy.wait()
            small[pl.ds(low, count)] += small_in[step, 0:count]
        small_done[pl.ds(low, count)] = small[pl.ds(low, count)]
        for back, (here, count, name, partner) in enumerate(reversed(halved)):
            slot = len(axes) + back
            span = small_done.at[pl.ds(low, count)]
            copy = remote(span, span, sm_send.at[slot], sm_recv.at[slot], {name: partner})
            copy.start()
            yield
            copy.wait()
            low = low - here * count
        for b in range(blocks):
            out_taps[:, cols(b)] = small_done[b, 0:tap_count, :] * scale
            out_gain[:, cols(b)] = small_done[b, tap_count : tap_count + 1, :] * scale
            out_shift[:, cols(b)] = small_done[b, tap_count + 1 : tap_count + 2, :] * scale

    flows = [exchange(k) for k in range(streams)]

    def advance():
        for flow in list(flows):
            if next(flow, "end") == "end":
                flows.remove(flow)

    for k in range(streams):
        for o in range(1, n_dp):
            peer = (dp + o) % n_dp
            dp_out[o - 1, k] = product(peer, k)
            copy = remote(
                dp_out.at[o - 1, k], dp_in.at[o - 1, k],
                dp_send.at[k, o - 1], dp_recv.at[k, o - 1], {"dp": peer},
            )
            copy.start()
            dp_copies[k][o - 1] = copy
        acc[k] = product(dp, k)

    for copy in w_copies:
        copy.wait()
    own.wait()
    total = None
    for d in range(n_dp):
        part = jnp.dot(cotan[:, d * local_rows : (d + 1) * local_rows], weights[d], preferred_element_type=f32)
        total = part if total is None else total + part
    grad_act[...] = total
    sums[...] = jnp.zeros_like(sums)

    def backward(i):
        r0 = pl.multiple_of(i * block_rows, block_rows)
        rows = pl.ds(r0, block_rows)
        inv_std = inv[rows, :]
        normal, grad_normal = [], []
        for b in range(blocks):
            n = normed[rows, cols(b)]
            pre = n * gain[:, cols(b)] + shift[:, cols(b)]
            s = jax.nn.sigmoid(pre)
            grad_pre = grad_act[rows, cols(b)] * s * (1.0 + pre * (1.0 - s))
            sums[0, b] += jnp.sum((grad_pre * n).reshape(block_rows // 8, 8, LANES), axis=0)
            sums[1, b] += jnp.sum(grad_pre.reshape(block_rows // 8, 8, LANES), axis=0)
            normal.append(n)
            grad_normal.append(grad_pre * gain[:, cols(b)])
        first = row_mean(grad_normal)
        second = row_mean([g * n for g, n in zip(grad_normal, normal)])
        for b in range(blocks):
            grads[b, rows, :] = inv_std * (grad_normal[b] - first - normal[b] * second)

    backward(0)
    edge_out[...] = grads[:, 0:ext, :]
    edge = remote(edge_out, edge_in, h_send.at[2], h_recv.at[2], {"sp": prior})
    edge.start()
    advance()

    def backward_loop(i, _):
        backward(i)
        return 0

    lax.fori_loop(1, row_blocks, backward_loop, 0)

    small[...] = jnp.zeros_like(small)
    for b in range(blocks):

        def tap_rows(i, carry):
            r0 = pl.multiple_of(i * 8, 8)
            g = grads[b, pl.ds(r0, 8), :]
            return tuple(c + g * gated[b, pl.ds(r0 + lead + j, 8), :] for j, c in enumerate(carry))

        found = lax.fori_loop(
            0, length // 8, tap_rows, tuple(jnp.zeros((8, LANES), f32) for _ in range(tap_count))
        )
        for j in range(tap_count):
            small[b, j : j + 1, :] = jnp.sum(found[j], axis=0, keepdims=True)
        for row in range(2):
            small[b, tap_count + row : tap_count + row + 1, :] = jnp.sum(sums[row, b], axis=0, keepdims=True)
    flows.insert(0, combine())
    edge.wait()
    for b in range(blocks):
        grads[b, pl.ds(length, ext), :] = jnp.where(sp < n_sp - 1, edge_in[b], 0.0)
    advance()

    def final_rows(i, _):
        r0 = pl.multiple_of(i * block_rows, block_rows)
        rows = pl.ds(r0, block_rows)
        for b in range(blocks):
            total = jnp.zeros((block_rows, LANES), f32)
            for j in range(tap_count):
                total = total + taps[j : j + 1, cols(b)] * grads[b, pl.ds(r0 + tap_count - 1 - j, block_rows), :]
            s = jax.nn.sigmoid(gate[rows, cols(b)].astype(f32))
            grad_value[rows, cols(b)] = (total * s).astype(bf16)
            grad_gate[rows, cols(b)] = (total * value[rows, cols(b)].astype(f32) * s * (1.0 - s)).astype(bf16)
        return 0

    pieces = math.gcd(row_blocks, 4)
    step = row_blocks // pieces
    for piece in range(pieces):
        lax.fori_loop(piece * step, (piece + 1) * step, final_rows, 0)
        advance()
    while flows:
        advance()


def per_device(glu_value, glu_gate, cotangent, conv_weight, norm_gain, norm_shift, out_weight):
    n_sp, n_dp = lax.axis_size("sp"), lax.axis_size("dp")
    length, channels = glu_value.shape[1:]
    features = cotangent.shape[2]
    tap_count = conv_weight.shape[0]
    local_rows = out_weight.shape[0]
    scale = 1.0 / math.sqrt(length * n_sp * n_dp)
    ext = -(-(tap_count - 1) // 16) * 16
    blocks = channels // LANES
    streams = STREAMS
    while streams > 1 and (local_rows // streams) % LANES:
        streams //= 2
    stream_rows = local_rows // streams
    plan, final = stage_plan(n_sp, stream_rows)
    full_rows = max([rows for halve, rows in plan if not halve] + [8])
    small_rows = -(-(tap_count + 2) // 8) * 8
    steps = int(math.log2(n_sp)) + int(math.log2(n_dp))
    dma = pltpu.SemaphoreType.DMA
    vmem = pltpu.VMEM
    peers = max(n_dp - 1, 1)
    spec = pl.BlockSpec(memory_space=pltpu.VMEM)
    grad_value, grad_gate, grad_weight, grad_conv, grad_gain, grad_shift = pl.pallas_call(
        functools.partial(kernel, n_sp, n_dp, plan, scale),
        out_shape=[
            jax.ShapeDtypeStruct((length, channels), bf16),
            jax.ShapeDtypeStruct((length, channels), bf16),
            jax.ShapeDtypeStruct((local_rows, channels), bf16),
            jax.ShapeDtypeStruct((tap_count, channels), f32),
            jax.ShapeDtypeStruct((1, channels), f32),
            jax.ShapeDtypeStruct((1, channels), f32),
        ],
        in_specs=[spec] * 7,
        out_specs=[spec] * 6,
        scratch_shapes=[
            vmem((blocks, ext + length, LANES), f32),
            vmem((blocks, length + ext, LANES), f32),
            vmem((length, channels), f32),
            vmem((length, 1), f32),
            vmem((length, channels), bf16),
            vmem((length, channels), f32),
            vmem((n_dp, local_rows, channels), bf16),
            vmem((ext, channels), bf16),
            vmem((ext, channels), bf16),
            vmem((blocks, ext, LANES), f32),
            vmem((blocks, ext, LANES), f32),
            vmem((2, blocks, 8, LANES), f32),
            vmem((blocks, small_rows, LANES), f32),
            vmem((steps, blocks, small_rows, LANES), f32),
            vmem((blocks, small_rows, LANES), f32),
            vmem((peers, streams, stream_rows, channels), f32),
            vmem((peers, streams, stream_rows, channels), f32),
            vmem((streams, stream_rows, channels), f32),
            vmem((streams, stream_rows, channels), bf16),
            vmem((streams, stream_rows, channels), bf16),
            vmem((streams, stream_rows, channels), f32),
            vmem((streams, len(plan), full_rows, channels), f32),
            vmem((local_rows, channels), bf16),
            dma,
            dma((peers,)), dma((peers,)),
            dma((3,)), dma((3,)),
            dma((streams, peers)), dma((streams, peers)),
            dma((streams, 2 * len(plan))), dma((streams, 2 * len(plan))),
            dma((2 * steps,)), dma((2 * steps,)),
        ],
        compiler_params=pltpu.CompilerParams(
            collective_id=0, has_side_effects=True, vmem_limit_bytes=60 * 1024 * 1024
        ),
    )(glu_value[0], glu_gate[0], cotangent[0], conv_weight, norm_gain[None], norm_shift[None], out_weight)
    return (
        grad_value[None],
        grad_gate[None],
        grad_weight.astype(f32) * scale,
        grad_conv,
        grad_gain[0],
        grad_shift[0],
    )


def solution(mesh):
    in_specs = (
        P("dp", "sp", None),
        P("dp", "sp", None),
        P("dp", "sp", None),
        P(),
        P(),
        P(),
        P("dp", None),
    )
    out_specs = (P("dp", "sp", None), P("dp", "sp", None), P("dp", None), P(), P(), P())
    return jax.shard_map(
        per_device, mesh=mesh, in_specs=in_specs, out_specs=out_specs, check_vma=False
    )
```
